32 devices in a mesh: fs: 8 (over z, x), tp: 4 (over y, core).
Axes of the slice: x: 2, y: 2, z: 4, core: 2. Of those that a mesh axis runs over, the one named last changes fastest.
Arguments:
- tokens: bfloat16 [4096, 2048], P('fs', 'tp'), may hold values from -6 to 6
- pre_gain: float32 [2048], P('fs'), may hold values from 0.1 to 1.9
- gate_weight: float32 [2048, 6144], P('fs', 'tp'), may hold values from -0.125 to 0.125
- up_weight: float32 [2048, 6144], P('fs', 'tp'), may hold values from -0.125 to 0.125
- down_weight: float32 [2048, 6144], P('fs', 'tp'), may hold values from -0.078125 to 0.078125
- post_gain: float32 [2048], P('tp'), may hold values from 0.1 to 1.9
Outputs:
- result: bfloat16 [4096, 2048], P('fs', 'tp')
- gate_ready: bfloat16 [2048, 6144], P(None, 'tp')
- up_ready: bfloat16 [2048, 6144], P(None, 'tp')
- down_ready: bfloat16 [2048, 6144], P(None, 'tp')
The draws below stay inside these ranges and needn't reach their ends.
All inputs are finite; a program needn't handle non-finite values.
Results may differ from the reference program's by a relative error of at most 0.015.
Values may be sent and summed in bfloat16 or wider, within the bound.
No kernel may reach another device: no remote copies, remote signals or barrier semaphores. Data moves between devices by JAX's collectives and lax.ppermute only.
A program may use at most 128 MiB of HBM per device.

```python
import jax
import jax.numpy as jnp
from jax import lax

D = 2048
FF = 6144
TOKENS = 4096


def levels(rng, shape, pieces, smallest, top_value):
    def one(position, blocks):
        heights = jax.random.uniform(jax.random.fold_in(jax.random.fold_in(rng, 6), position), (blocks,), jnp.float32, smallest / len(pieces), top_value / len(pieces))
        return jnp.repeat(jnp.exp(heights), shape[position] // blocks).reshape((-1,) + (1,) * (len(shape) - position - 1))

    loudness = one(*pieces[0])
    for cut in pieces[1:]:
        loudness = loudness * one(*cut)
    return loudness


def bell_draw(stream_key, extent, spread, reach, cuts=(), kind=jnp.bfloat16):
    drawn = jax.random.normal(stream_key, extent, jnp.float32) * spread
    if len(cuts) > 0:
        drawn = levels(stream_key, extent, cuts, -0.22, 0.18) * drawn
    return jnp.clip(drawn, min=-reach, max=reach).astype(kind)


def setup_inputs(seed: int = 0) -> dict:
    keys = jax.random.split(jax.random.key(seed), 7)
    return {
        "tokens": bell_draw(keys[0], (TOKENS, D), 1.0, 6.0, ((0, 8), (1, 4))),
        "pre_gain": jnp.clip(1.0 + 0.18 * jax.random.normal(keys[1], (D,), jnp.float32), 0.1, 1.9),
        "gate_weight": bell_draw(keys[2], (D, FF), D ** -0.5, 0.125, ((0, 8), (1, 4)), jnp.float32),
        "up_weight": bell_draw(keys[3], (D, FF), D ** -0.5, 0.125, ((0, 8), (1, 4)), jnp.float32),
        "down_weight": bell_draw(keys[4], (D, FF), FF ** -0.5, 0.078125, ((0, 8), (1, 4)), jnp.float32),
        "post_gain": jnp.clip(1.0 + 0.18 * jax.random.normal(keys[5], (D,), jnp.float32), 0.1, 1.9),
    }


EPS = 1e-06

def reference(tokens, pre_gain, gate_weight, up_weight, down_weight, post_gain):
    gate_ready = (pre_gain[:, None] * gate_weight).astype(jnp.bfloat16)
    up_ready = (pre_gain[:, None] * up_weight).astype(jnp.bfloat16)
    down_ready = down_weight.astype(jnp.bfloat16)
    widened = tokens.astype(jnp.float32)
    normalized = (widened * lax.rsqrt(lax.optimization_barrier(jnp.mean(widened * widened, axis=1, keepdims=True)) + EPS)).astype(jnp.bfloat16)
    gate = jnp.dot(normalized, gate_ready, preferred_element_type=jnp.float32)
    up = jnp.dot(normalized, up_ready, preferred_element_type=jnp.float32)
    hidden = (jax.nn.silu(gate) * up).astype(jnp.bfloat16)
    mixed = lax.dot_general(hidden, down_ready, (((1,), (1,)), ((), ())), preferred_element_type=jnp.float32)
    scaling = lax.rsqrt(lax.optimization_barrier(jnp.mean(mixed * mixed, axis=1, keepdims=True)) + EPS)
    result = (mixed * scaling * post_gain[None, :]).astype(jnp.bfloat16)
    return (result, gate_ready, up_ready, down_ready)
```

```python
import jax
import jax.numpy as jnp
import numpy as np
from jax import lax
from jax.sharding import PartitionSpec as P

EPS = 1e-06


def ring_order(mesh):
    line = list(mesh.devices[:, 0])
    n = len(line)
    coords = [getattr(d, "coords", None) for d in line]
    if any(c is None for c in coords):
        return list(range(n))
    varying = [a for a in range(len(coords[0])) if len({c[a] for c in coords}) > 1]
    if len(varying) != 2:
        return list(range(n))
    at = {tuple(c[a] for a in varying): i for i, c in enumerate(coords)}
    for flip in (False, True):
        first = sorted({p[1 if flip else 0] for p in at})
        second = sorted({p[0 if flip else 1] for p in at})
        if len(first) * len(second) != n or len(second) % 2:
            continue
        cells = [(u, second[0]) for u in first[:1]]
        cells = [(first[0], v) for v in second]
        for k, v in enumerate(reversed(second)):
            rest = first[1:] if k % 2 == 0 else first[:0:-1]
            cells += [(u, v) for u in rest]
        return [at[(v, u) if flip else (u, v)] for u, v in cells]
    return list(range(n))


def after(value, *others):
    return lax.optimization_barrier((value, *others))[0]


def make_shards(mesh):
    n, m = mesh.shape["fs"], mesh.shape["tp"]
    ring = ring_order(mesh)
    forward = [(ring[i], ring[(i + 1) % n]) for i in range(n)]
    backward = [(b, a) for a, b in forward]
    position = {d: p for p, d in enumerate(ring)}
    source = np.array(
        [[ring[(position[d] - k) % n] for k in range(n)] for d in range(n)], np.int32
    )
    far = n // 2

    def turn(value, r):
        return lax.ppermute(value, "tp", [(j, (j + r) % m) for j in range(m)])

    def shards(tokens, pre_gain, gate_weight, up_weight, down_weight, post_gain):
        me, tp = lax.axis_index("fs"), lax.axis_index("tp")
        origin = lax.dynamic_index_in_dim(jnp.asarray(source), me, 0, keepdims=False)
        rows = gate_weight.shape[0]
        half = rows // 2
        gate_local = (pre_gain[:, None] * gate_weight).astype(jnp.bfloat16)
        up_local = (pre_gain[:, None] * up_weight).astype(jnp.bfloat16)
        down_local = down_weight.astype(jnp.bfloat16)

        def hop(value, way):
            return lax.ppermute(value, "fs", forward if way > 0 else backward)

        def rounds(a, b, gates):
            got = {("a", 0): a, ("b", 0): b}
            order = {1: [], -1: []}
            for k in range(1, far + 1):
                for way, names in ((1, "ab"), (-1, "ba")):
                    for name in names if k < far else names[0]:
                        previous = got[(name, way * (k - 1))]
                        if k == 1:
                            previous = after(previous, *gates[way][len(order[way])])
                        got[(name, way * k)] = hop(previous, way)
                        order[way].append(got[(name, way * k)])
            return got, order

        none = {1: [(), ()], -1: [(), ()]}
        wide, order = rounds(gate_local, up_local, none)
        later = {w: [(order[w][-2],), (order[w][-1],)] for w in (1, -1)}
        narrow, _ = rounds(down_local[:half], down_local[half:], later)

        width = tokens.shape[1] * m
        whole = jnp.zeros((tokens.shape[0], width), tokens.dtype)
        whole = lax.dynamic_update_slice(whole, tokens, (0, tp * tokens.shape[1]))
        for r in range(1, m):
            whole = lax.dynamic_update_slice(
                whole, turn(tokens, r), (0, ((tp - r) % m) * tokens.shape[1])
            )
        widened = whole.astype(jnp.float32)
        normalized = (
            widened * lax.rsqrt(jnp.mean(widened * widened, axis=1, keepdims=True) + EPS)
        ).astype(jnp.bfloat16)

        def place(full, piece, k, offset=0):
            return lax.dynamic_update_slice(full, piece, (origin[k % n] * rows + offset, 0))

        full = (rows * n, gate_weight.shape[1])
        gate_full, up_full, down_full = (jnp.zeros(full, jnp.bfloat16) for _ in range(3))
        gate_full = place(gate_full, gate_local, 0)
        up_full = place(up_full, up_local, 0)
        down_full = place(down_full, down_local, 0)
        for (name, k), piece in wide.items():
            if k != 0:
                if name == "a":
                    gate_full = place(gate_full, piece, k)
                else:
                    up_full = place(up_full, piece, k)
        for (name, k), piece in narrow.items():
            if k != 0:
                down_full = place(down_full, piece, k, 0 if name == "a" else half)

        gate = jnp.dot(normalized, gate_full, preferred_element_type=jnp.float32)
        up = jnp.dot(normalized, up_full, preferred_element_type=jnp.float32)
        hidden = (jax.nn.silu(gate) * up).astype(jnp.bfloat16)

        contract = (((1,), (1,)), ((), ()))

        def share_of(piece):
            return lax.dot_general(
                hidden, piece, contract, preferred_element_type=jnp.float32
            ).astype(jnp.bfloat16)

        part = tokens.shape[0] // m

        def quarter(value, j):
            return lax.dynamic_slice_in_dim(value, j * part, part, 0)

        def reduce_over_tp(share):
            total = quarter(share, tp).astype(jnp.float32)
            for r in range(1, m):
                total = total + turn(quarter(share, (tp + r) % m), r).astype(jnp.float32)
            mine = total.astype(jnp.bfloat16)
            out = jnp.zeros(share.shape, jnp.bfloat16)
            out = lax.dynamic_update_slice_in_dim(out, mine, tp * part, 0)
            for r in range(1, m):
                out = lax.dynamic_update_slice_in_dim(out, turn(mine, r), ((tp - r) % m) * part, 0)
            return out

        mixed = jnp.zeros((tokens.shape[0], width), jnp.bfloat16)
        squares = jnp.zeros((tokens.shape[0], 1), jnp.float32)

        def take(mixed, squares, chunk, k, offset=0):
            wide_chunk = chunk.astype(jnp.float32)
            squares = squares + jnp.sum(wide_chunk * wide_chunk, axis=1, keepdims=True)
            mixed = lax.dynamic_update_slice(
                mixed, chunk.astype(jnp.bfloat16), (0, origin[k % n] * rows + offset)
            )
            return mixed, squares

        done = reduce_over_tp(share_of(down_local))
        mixed, squares = take(mixed, squares, done, 0)
        for k in range(1, far):
            both = [jnp.concatenate([narrow[("a", s * k)], narrow[("b", s * k)]]) for s in (1, -1)]
            done = reduce_over_tp(jnp.concatenate([share_of(b) for b in both], axis=1))
            mixed, squares = take(mixed, squares, done[:, :rows], k)
            mixed, squares = take(mixed, squares, done[:, rows:], -k)
        last = jnp.concatenate([narrow[("a", far)], narrow[("b", -far)]])
        share = share_of(last)
        total = share.astype(jnp.float32)
        for r in range(1, m):
            total = total + turn(share, r).astype(jnp.float32)
        mixed, squares = take(mixed, squares, total, far)

        scaling = lax.rsqrt(squares / width + EPS)
        mine = lax.dynamic_slice_in_dim(mixed, tp * tokens.shape[1], tokens.shape[1], 1)
        result = (mine.astype(jnp.float32) * scaling * post_gain[None, :]).astype(jnp.bfloat16)
        return (result, gate_full, up_full, down_full)

    return shards


def solution(mesh):
    return jax.shard_map(
        make_shards(mesh),
        mesh=mesh,
        in_specs=(P("fs", "tp"), P("fs"), P("fs", "tp"), P("fs", "tp"), P("fs", "tp"), P("tp")),
        out_specs=(P("fs", "tp"), P(None, "tp"), P(None, "tp"), P(None, "tp")),
        check_vma=False,
    )
```
